32 devices in a mesh: ep: 4 (over z), tp: 8 (over y, x, core).
Axes of the slice: x: 2, y: 2, z: 4, core: 2. Of those that a mesh axis runs over, the one named last changes fastest.
Arguments:
- tokens: bfloat16 [640, 2048], P('ep', 'tp'), may hold values from -6 to 6
- cotangent: bfloat16 [640, 2048], P('ep', 'tp'), may hold values from -6 to 6
- routes: int32 [640, 2], P('ep'), may hold values from 0 to 23, all different within a row; in each aligned block of 160 rows (0 to 159, 160 to 319, ...) at most 14 rows name the same one
- gate_weights: float32 [640, 2], P('ep'), may hold values from 0.2 to 2.5
- expert_gate: bfloat16 [24, 2048, 512], P('ep', 'tp'), may hold values from -0.125 to 0.125
- expert_up: bfloat16 [24, 2048, 512], P('ep', 'tp'), may hold values from -0.125 to 0.125
- expert_down: bfloat16 [24, 512, 2048], P('ep', None, 'tp'), may hold values from -0.25 to 0.25
- shared_gate: bfloat16 [2048, 576], P('tp'), may hold values from -0.125 to 0.125
- shared_up: bfloat16 [2048, 576], P('tp'), may hold values from -0.125 to 0.125
- shared_down: bfloat16 [576, 2048], P(None, 'tp'), may hold values from -0.25 to 0.25
Outputs:
- token_grad: bfloat16 [640, 2048], P('ep', 'tp')
- weight_grad: float32 [640, 2], P('ep')
- expert_gate_grad: float32 [24, 2048, 512], P('ep', 'tp')
- expert_up_grad: float32 [24, 2048, 512], P('ep', 'tp')
- expert_down_grad: float32 [24, 512, 2048], P('ep', None, 'tp')
- shared_gate_grad: float32 [2048, 576], P('tp', 'ep')
- shared_up_grad: float32 [2048, 576], P('tp', 'ep')
- shared_down_grad: float32 [576, 2048], P('ep', 'tp')
- gate_rows_sq: float32 [24, 2048], P('ep', 'tp')
- up_rows_sq: float32 [24, 2048], P('ep', 'tp')
- down_rows_sq: float32 [24, 512], P('ep')
- shared_gate_rows_sq: float32 [2048], P('tp')
- shared_up_rows_sq: float32 [2048], P('tp')
- shared_down_rows_sq: float32 [576], P('ep')
The draws below stay inside these ranges and needn't reach their ends.
Inputs may be any that keep to these rules, and one draw needn't show every extreme that they name: `routes`: each row names 2 different experts. Among the rows of one index of ep (aligned blocks of 160 rows) no expert is named more than 14 times, a bound that some block reaches.
All inputs are finite; a program needn't handle non-finite values.
Results may differ from the reference program's by a relative error of at most 0.0059.
Values may be sent and summed in bfloat16 or wider, within the bound.
A program may use at most 64 MiB of HBM per device.

```python
import math
import jax
import jax.numpy as jnp
import numpy as np
from jax import lax

D = 2048
FF = 512
SF = 576
TOP = 2
TOK_DEV = 160
EXPERTS = 24
CAP = 14
TOKENS = 640
N_EP = 4


def levels(key, shape, cuts, smallest, top_value):
    def one(axis_at, parts):
        heights = jax.random.uniform(jax.random.fold_in(jax.random.fold_in(key, 6), axis_at), (parts,), jnp.float32, smallest / len(cuts), top_value / len(cuts))
        return jnp.repeat(jnp.exp(heights), shape[axis_at] // parts).reshape((-1,) + (1,) * (len(shape) - axis_at - 1))

    loudness = one(*cuts[0])
    for cut in cuts[1:]:
        loudness = loudness * one(*cut)
    return loudness


def deal_out(stream_key, own, number, rows, number_of, top, bound, lean):
    order = jax.random.permutation(stream_key, number_of)
    packed, usual = load_shares(number_of, rows * top, bound, lean, True), load_shares(number_of, rows * top, bound, lean, False)
    places = jnp.arange(number_of)

    def named(sizes, rotation):
        used = int((sizes > 0).sum())
        fixed = max(1, used // 4)
        passed = fixed + (places - fixed + rotation * (used - fixed)) % max(1, number_of - fixed)
        return jnp.zeros((number_of,), jnp.int32).at[order[jnp.where(places < fixed, places, passed)]].set(jnp.asarray(sizes, jnp.int32))

    sizes = jnp.where(number % 4 == 0, named(packed, number // 4), named(usual, number - number // 4 - 1))
    mixed = jax.random.permutation(jax.random.fold_in(own, 3), number_of)
    source_of, receiver = mixed[0:number_of // 2 * 2:2], mixed[1:number_of // 2 * 2:2]
    room = jnp.minimum(sizes[source_of] - 1, bound - sizes[receiver]) // 2
    room = jnp.where((source_of == order[0]) | (receiver == order[0]) | (sizes[receiver] == 0), 0, jnp.maximum(room, 0))
    passed = jax.random.randint(jax.random.fold_in(own, 4), (number_of // 2,), 0, 1 << 20) % (room + 1)
    sizes = sizes.at[source_of].add(-passed).at[receiver].add(passed)
    labels = jnp.searchsorted(jnp.cumsum(sizes), jnp.arange(rows * top), side="right").astype(jnp.int32)
    listing = labels.reshape(top, rows).T
    listing = listing[jax.random.permutation(jax.random.fold_in(own, 1), rows)]
    rotation = jax.random.randint(jax.random.fold_in(own, 2), (rows, 1), 0, top)
    return jnp.take_along_axis(listing, (jnp.arange(top)[None, :] + rotation) % top, axis=1)


def load_shares(count, total, limit, skew, full):
    portions = [(1 << 20) // math.isqrt(grade ** skew) + 1 for grade in range(1, count + 1)]
    largest = limit if full else min(limit, max(-(-total // count), total * portions[0] // sum(portions)))
    least = 1 if total - largest >= count - 1 else 0
    holding, rest = [largest] + [least] * (count - 1), total - largest - least * (count - 1)
    while rest > 0:
        movable = [i for i in range(1, count) if holding[i] < largest] or [i for i in range(1, count) if holding[i] < limit]
        mass, left = sum([portions[i] for i in movable]), rest
        for i in movable:
            more = min(limit - holding[i], max(1, left * portions[i] // mass), rest)
            holding[i] = holding[i] + more
            rest = rest - more
    return np.array(holding)


def noise(rng, dims, spread, bound, split=(), held_as=jnp.bfloat16):
    entries = spread * jax.random.normal(rng, dims, jnp.float32)
    if split:
        entries = entries * levels(rng, dims, split, -0.22, 0.18)
    return jnp.clip(entries, -bound, bound).astype(held_as)


def setup_inputs(seed: int = 0) -> dict:
    seeds = jax.random.split(jax.random.key(seed), 11)
    tokens = noise(seeds[0], (TOKENS, D), 1.0, 6.0, ((0, 4), (1, 8)))
    cotangent = noise(seeds[1], (TOKENS, D), 1.0, 6.0, ((0, 4), (1, 8)))
    routes_keys = jax.random.split(jax.random.fold_in(seeds[2], 1), TOKENS // TOK_DEV)
    routes_turns = jax.random.permutation(jax.random.fold_in(seeds[2], 3), TOKENS // TOK_DEV)
    routes = jax.vmap(lambda own, number: deal_out(jax.random.fold_in(seeds[2], 2), own, number, TOK_DEV, EXPERTS, TOP, CAP, 1))(routes_keys, routes_turns).reshape((TOKENS, TOP))
    gate_weights = jnp.clip(jnp.exp(math.log(2.5) - 2.5257286 * jax.random.uniform(seeds[3], (TOKENS, TOP), jnp.float32) ** levels(seeds[3], (TOKENS, TOP), ((0, 4),), -0.2, 0.2)), 0.2, 2.5)
    expert_gate = noise(seeds[4], (EXPERTS, D, FF), D ** -0.5, 0.125, ((0, 4), (1, 8)))
    expert_up = noise(seeds[5], (EXPERTS, D, FF), D ** -0.5, 0.125, ((0, 4), (1, 8)))
    expert_down = noise(seeds[6], (EXPERTS, FF, D), FF ** -0.5, 0.25, ((0, 4), (2, 8)))
    shared_gate = noise(seeds[7], (D, SF), D ** -0.5, 0.125, ((0, 8),))
    shared_up = noise(seeds[8], (D, SF), D ** -0.5, 0.125, ((0, 8),))
    shared_down = noise(seeds[9], (SF, D), SF ** -0.5, 0.25, ((1, 8),))
    return {"tokens": tokens, "cotangent": cotangent, "routes": routes, "gate_weights": gate_weights, "expert_gate": expert_gate, "expert_up": expert_up, "expert_down": expert_down, "shared_gate": shared_gate, "shared_up": shared_up, "shared_down": shared_down}


def silu_parts(pre):
    logistic = jax.nn.sigmoid(pre)
    return pre * logistic, logistic * (1.0 + pre * (1.0 - logistic))


def contract(left, right, left_dim, right_dim):
    return lax.dot_general(left, right, (((left_dim,), (right_dim,)), ((), ())), preferred_element_type=jnp.float32)


def reference(tokens, cotangent, routes, gate_weights, expert_gate, expert_up, expert_down, shared_gate, shared_up, shared_down):
    assigned = TOK_DEV * TOP
    owners = routes.reshape(N_EP, assigned).astype(jnp.int32)
    picked = (owners[:, :, None] == jnp.arange(EXPERTS, dtype=jnp.int32)[None, None, :]).astype(jnp.int32)
    slot_rank = jnp.sum((jnp.cumsum(picked, axis=1) - picked) * picked, axis=2).astype(jnp.int32)
    block_ids = jnp.arange(N_EP, dtype=jnp.int32)[:, None]
    global_tok = block_ids * TOK_DEV + (jnp.arange(assigned, dtype=jnp.int32) // TOP)[None, :]
    row_index = block_ids * CAP + slot_rank
    table = jnp.full((EXPERTS, N_EP * CAP), TOKENS, jnp.int32).at[owners, row_index].set(global_tok)
    weight_table = jnp.zeros((EXPERTS, N_EP * CAP), jnp.float32).at[owners, row_index].set(gate_weights.reshape(N_EP, assigned))
    zero_row = jnp.zeros((1, D), jnp.bfloat16)
    padded_tok = jnp.concatenate([tokens, zero_row], axis=0)
    padded_cot = jnp.concatenate([cotangent, zero_row], axis=0)

    def one_expert(inputs):
        chosen, weights, w_gate, w_up, w_down = inputs
        rows_x = padded_tok[chosen]
        rows_dy = padded_cot[chosen]
        gate_pre = jnp.dot(rows_x, w_gate, preferred_element_type=jnp.float32)
        up_pre = jnp.dot(rows_x, w_up, preferred_element_type=jnp.float32)
        back = contract(rows_dy, w_down, 1, 1)
        silu_out, silu_slope = silu_parts(gate_pre)
        hidden = (silu_out * up_pre).astype(jnp.bfloat16)
        dhidden = weights[:, None] * back
        grad_gate = (dhidden * up_pre * silu_slope).astype(jnp.bfloat16)
        grad_up = (dhidden * silu_out).astype(jnp.bfloat16)
        weighted = (weights[:, None] * rows_dy.astype(jnp.float32)).astype(jnp.bfloat16)
        gate_grad = jnp.sum(hidden.astype(jnp.float32) * back, axis=1)
        down_grad = contract(hidden, weighted, 0, 0)
        gate_wgrad = contract(rows_x, grad_gate, 0, 0)
        up_wgrad = contract(rows_x, grad_up, 0, 0)
        row_grad = contract(grad_gate, w_gate, 1, 1) + contract(grad_up, w_up, 1, 1)
        return gate_wgrad, up_wgrad, down_grad, row_grad.astype(jnp.bfloat16), gate_grad

    gate_wgrads, up_wgrads, down_grads, row_grads, gate_grads = lax.map(
        one_expert, (table, weight_table, expert_gate, expert_up, expert_down))
    routed = row_grads[owners, row_index].astype(jnp.float32).reshape(TOKENS, TOP, D).sum(axis=1)
    weight_grad = gate_grads[owners, row_index].reshape(TOKENS, TOP)

    s_gate = jnp.dot(tokens, shared_gate, preferred_element_type=jnp.float32)
    s_up = jnp.dot(tokens, shared_up, preferred_element_type=jnp.float32)
    s_back = contract(cotangent, shared_down, 1, 1)
    s_out, s_slope = silu_parts(s_gate)
    s_hidden = (s_out * s_up).astype(jnp.bfloat16)
    s_dgate = (s_back * s_up * s_slope).astype(jnp.bfloat16)
    s_dup = (s_back * s_out).astype(jnp.bfloat16)
    shared_gate_grad = contract(tokens, s_dgate, 0, 0)
    shared_up_grad = contract(tokens, s_dup, 0, 0)
    shared_down_grad = contract(s_hidden, cotangent, 0, 0)
    shared_rows = contract(s_dgate, shared_gate, 1, 1) + contract(s_dup, shared_up, 1, 1)
    token_grad = (routed + shared_rows).astype(jnp.bfloat16)
    return (token_grad, weight_grad, gate_wgrads, up_wgrads, down_grads,
            shared_gate_grad, shared_up_grad, shared_down_grad,
            jnp.sum(gate_wgrads * gate_wgrads, axis=2), jnp.sum(up_wgrads * up_wgrads, axis=2),
            jnp.sum(down_grads * down_grads, axis=2),
            jnp.sum(shared_gate_grad * shared_gate_grad, axis=1),
            jnp.sum(shared_up_grad * shared_up_grad, axis=1),
            jnp.sum(shared_down_grad * shared_down_grad, axis=1))
```

```python
import functools

import jax
import jax.numpy as jnp
from jax import lax
from jax.experimental import pallas as pl
from jax.experimental.pallas import tpu as pltpu
from jax.sharding import PartitionSpec as P

BF = jnp.bfloat16
F32 = jnp.float32
MESH = pl.DeviceIdType.MESH
VMEM = pl.BlockSpec(memory_space=pltpu.VMEM)


def up_to(value, unit):
    return (value + unit - 1) // unit * unit


def silu_parts(pre):
    logistic = jax.nn.sigmoid(pre)
    return (pre * logistic, logistic * (1.0 + pre * (1.0 - logistic)))


def remote(src, dst, send, recv, where):
    return pltpu.make_async_remote_copy(
        src_ref=src,
        dst_ref=dst,
        send_sem=send,
        recv_sem=recv,
        device_id=where,
        device_id_type=MESH,
    )


def greet(places):
    barrier = pltpu.get_barrier_semaphore()
    for place in places:
        pl.semaphore_signal(barrier, inc=1, device_id=place, device_id_type=MESH)
    pl.semaphore_wait(barrier, len(places))


def gather_kernel(n_ep, x, dy, meta, all_x, all_dy, all_meta, send, recv):
    me = lax.axis_index("ep")
    peers = [lax.rem(me + d, n_ep) for d in range(1, n_ep)]
    greet([{"ep": p} for p in peers])
    pairs = ((meta, all_meta), (x, all_x), (dy, all_dy))
    copies = []
    for d, p in enumerate(peers):
        for k, (src, dst) in enumerate(pairs):
            c = remote(src, dst.at[me], send.at[d, k], recv.at[d, k], {"ep": p})
            c.start()
            copies.append(c)
    for src, dst in pairs:
        dst[me] = src[...]
    for c in copies:
        c.wait()


def hidden_kernel(
    n_tp, cols, g, u, b, s, rw, hid, gg, gu, so, dots,
    pg, pu, pb, ps, hg, hu, hb, hs, cg, cu, cb, cs,
    a_send, a_recv, b_send, b_recv, c_send, c_recv, d_send, d_recv,
):
    me = lax.axis_index("tp")
    half = n_tp // 2
    parity = lax.rem(me, 2)
    mine = me // 2
    partner = {"tp": me + 1 - 2 * parity}
    others = [lax.rem(mine + d, half) for d in range(1, half)]
    places = [{"tp": 2 * j + parity} for j in others]
    rows = g.shape[0] // n_tp
    s_rows = s.shape[0] // n_tp
    greet([partner] + places)

    full = (s, g, u, b)
    got = (ps, pg, pu, pb)
    held = (hs, hg, hu, hb)
    landed = (cs, cg, cu, cb)
    sizes = (s_rows, rows, rows, rows)

    def span(start, size):
        return pl.ds(pl.multiple_of(start * size, size), size)

    first = []
    for k in range(4):
        c = remote(
            full[k].at[span(1 - parity, half * sizes[k])],
            got[k],
            a_send.at[k],
            a_recv.at[k],
            partner,
        )
        c.start()
        first.append(c)
    second = []
    for k in range(4):
        first[k].wait()
        held[k][...] = (
            full[k][span(parity, half * sizes[k]), :].astype(F32) + got[k][...].astype(F32)
        ).astype(BF)
        for d, j in enumerate(others):
            c = remote(
                held[k].at[span(j, sizes[k])],
                landed[k].at[d],
                b_send.at[d, k],
                b_recv.at[d, k],
                places[d],
            )
            c.start()
            second.append(c)

    place = parity * half + mine

    def total(k):
        for d in range(half - 1):
            second[k * (half - 1) + d].wait_recv()
        out = full[k][span(place, sizes[k]), :].astype(F32)
        out = out + got[k][span(mine, sizes[k]), :].astype(F32)
        for d in range(half - 1):
            out = out + landed[k][d].astype(F32)
        return out

    last = []

    def share(k, ref, where):
        block = ref.at[where]
        c = remote(block, block, d_send.at[0, k], d_recv.at[0, k], partner)
        c.start()
        last.append(c)
        for d in range(half - 1):
            c = remote(block, block, c_send.at[d, k], c_recv.at[d, k], places[d])
            c.start()
            last.append(c)

    both = total(0)
    width = both.shape[1]
    lane = lax.broadcasted_iota(jnp.int32, both.shape, 1)
    s_up = pltpu.roll(both, width - cols, 1)
    s_back = pltpu.roll(both, width - 2 * cols, 1)
    s_out, s_slope = silu_parts(both)
    s_hidden = s_out * s_up
    s_dgate = pltpu.roll(s_back * s_up * s_slope, cols, 1)
    s_dup = pltpu.roll(s_back * s_out, 2 * cols, 1)
    so[span(place, s_rows), :] = jnp.where(
        lane < cols, s_hidden, jnp.where(lane < 2 * cols, s_dgate, s_dup)
    ).astype(BF)
    share(0, so, span(place, s_rows))

    gate, up, back = total(1), total(2), total(3)
    silu_out, silu_slope = silu_parts(gate)
    hidden = (silu_out * up).astype(BF)
    dhidden = rw[span(place, rows), :][:, :1] * back
    mine_rows = span(place, rows)
    hid[mine_rows, :] = hidden
    gg[mine_rows, :] = (dhidden * up * silu_slope).astype(BF)
    gu[mine_rows, :] = (dhidden * silu_out).astype(BF)
    dots[place] = lax.dot_general(
        jnp.ones((8, gate.shape[1]), F32),
        hidden.astype(F32) * back,
        (((1,), (1,)), ((), ())),
        precision=lax.Precision.HIGHEST,
        preferred_element_type=F32,
    )
    outs = ((so, s_rows), (hid, rows), (gg, rows), (gu, rows), (dots, 1))
    for k in range(1, 4):
        share(k, outs[k][0], mine_rows)
    share(4, dots, pl.ds(place, 1))

    for k, (ref, size) in enumerate(outs):
        for d in range(half - 1):
            source = lax.rem(mine + half - 1 - d, half)
            at = parity * half + source
            where = pl.ds(at, 1) if k == 4 else span(at, size)
            block = ref.at[where]
            remote(
                block, block, c_send.at[d, k], c_recv.at[d, k], places[d]
            ).wait_recv()
            c = remote(block, block, d_send.at[1 + d, k], d_recv.at[1 + d, k], partner)
            c.start()
            last.append(c)
    for c in second:
        c.wait_send()
    for k, (ref, size) in enumerate(outs):
        for d in range(half):
            source = mine if d == 0 else lax.rem(mine + half - d, half)
            at = (1 - parity) * half + source
            where = pl.ds(at, 1) if k == 4 else span(at, size)
            block = ref.at[where]
            remote(block, block, d_send.at[d, k], d_recv.at[d, k], partner).wait_recv()
    for c in last:
        c.wait_send()


def finish_kernel(
    n_ep, n_tp, tg, wg, es, ts, token_out, wg_out, es_out, ts_out,
    tg_in, wg_in, es_in, ts_in, e_send, e_recv, t_send, t_recv,
):
    ep, tp = lax.axis_index("ep"), lax.axis_index("tp")
    eps = [lax.rem(ep + d, n_ep) for d in range(1, n_ep)]
    tps = [lax.rem(tp + d, n_tp) for d in range(1, n_tp)]
    greet([{"ep": p} for p in eps] + [{"tp": p} for p in tps])
    copies = []
    for d, p in enumerate(eps):
        for k, (src, dst) in enumerate(
            ((tg.at[p], tg_in.at[d]), (wg.at[p], wg_in.at[d]), (es, es_in.at[d]))
        ):
            copies.append(remote(src, dst, e_send.at[d, k], e_recv.at[d, k], {"ep": p}))
            copies[-1].start()
    for d, p in enumerate(tps):
        copies.append(remote(ts, ts_in.at[d], t_send.at[d], t_recv.at[d], {"tp": p}))
        copies[-1].start()
    for c in copies:
        c.wait()
    rows = tg[ep].astype(F32)
    weights = wg[ep]
    norms = es[...]
    for d in range(n_ep - 1):
        rows = rows + tg_in[d].astype(F32)
        weights = weights + wg_in[d]
        norms = norms + es_in[d]
    token_out[...] = rows.astype(BF)
    wg_out[...] = weights
    es_out[...] = norms
    down = ts[...]
    for d in range(n_tp - 1):
        down = down + ts_in[d]
    ts_out[...] = down


def call(kernel, collective, outs, scratch, *args):
    return pl.pallas_call(
        kernel,
        out_shape=[jax.ShapeDtypeStruct(s, t) for s, t in outs],
        in_specs=[VMEM] * len(args),
        out_specs=[VMEM] * len(outs),
        scratch_shapes=scratch,
        compiler_params=pltpu.CompilerParams(
            collective_id=collective,
            has_side_effects=True,
            vmem_limit_bytes=48 * 1024 * 1024,
        ),
    )(*args)


def per_device(
    n_ep, n_tp,
    tokens, cotangent, routes, gate_weights,
    expert_gate, expert_up, expert_down,
    shared_gate, shared_up, shared_down,
):
    dma = pltpu.SemaphoreType.DMA
    half = n_tp // 2
    tok_rows, narrow = tokens.shape
    picks = routes.shape[1]
    experts, _, ff = expert_gate.shape
    experts_all = experts * n_ep
    capacity = max(2, (tok_rows * picks + experts_all - 1) // experts_all)
    every = tok_rows * n_ep
    sf = shared_gate.shape[1]
    cols = sf // n_ep
    ep = lax.axis_index("ep")

    meta = jnp.concatenate([routes.astype(F32), gate_weights], axis=1).T
    meta = jnp.pad(meta, ((0, up_to(2 * picks, 8) - 2 * picks), (0, 0)))
    all_x, all_dy, all_meta = call(
        functools.partial(gather_kernel, n_ep),
        0,
        [
            ((n_ep, tok_rows, narrow), BF),
            ((n_ep, tok_rows, narrow), BF),
            ((n_ep,) + meta.shape, F32),
        ],
        [dma((n_ep - 1, 3)), dma((n_ep - 1, 3))],
        tokens, cotangent, meta,
    )
    all_x = all_x.reshape(every, narrow)
    all_dy = all_dy.reshape(every, narrow)

    ids = (ep * experts + jnp.arange(experts, dtype=jnp.int32)).astype(F32)
    match = all_meta[:, :picks, None, :] == ids[None, None, :, None]
    chosen = jnp.any(match, axis=1)
    weight_of = jnp.sum(
        jnp.where(match, all_meta[:, picks : 2 * picks, None, :], 0.0), axis=1
    )
    before = jnp.triu(jnp.ones((tok_rows, tok_rows), BF), 1)
    rank = jnp.einsum(
        "bet,ts->bes", chosen.astype(BF), before, preferred_element_type=F32
    ).astype(jnp.int32)
    slot = jnp.where(
        chosen,
        rank + capacity * jnp.arange(n_ep, dtype=jnp.int32)[:, None, None],
        -1,
    )
    per_expert = up_to(capacity * n_ep, 16)
    used = experts * per_expert
    rows = up_to(used, 16 * n_tp)
    slot = slot.transpose(1, 0, 2).reshape(experts, 1, every)
    hot = slot == jnp.arange(per_expert, dtype=jnp.int32)[None, :, None]
    onehot = hot.astype(BF)
    row_weight = jnp.sum(
        jnp.where(hot, weight_of.transpose(1, 0, 2).reshape(experts, 1, every), 0.0), axis=2
    )
    recv_x = jnp.einsum("ert,tl->erl", onehot, all_x, preferred_element_type=BF)
    recv_dy = jnp.einsum("ert,tl->erl", onehot, all_dy, preferred_element_type=BF)

    def flat(a):
        return jnp.pad(a.reshape(used, a.shape[-1]), ((0, rows - used), (0, 0)))

    gate_part = flat(jnp.einsum("erl,elf->erf", recv_x, expert_gate, preferred_element_type=BF))
    up_part = flat(jnp.einsum("erl,elf->erf", recv_x, expert_up, preferred_element_type=BF))
    back_part = flat(jnp.einsum("erl,efl->erf", recv_dy, expert_down, preferred_element_type=BF))
    s_pair = jnp.concatenate(
        [
            lax.dynamic_slice_in_dim(shared_gate, ep * cols, cols, 1),
            lax.dynamic_slice_in_dim(shared_up, ep * cols, cols, 1),
        ],
        axis=1,
    )
    s_down = lax.dynamic_slice_in_dim(shared_down, ep * cols, cols, 0)
    width = up_to(3 * cols, 128)
    s_part = jnp.concatenate(
        [
            jnp.dot(all_x, s_pair, preferred_element_type=BF),
            jnp.einsum("tl,sl->ts", all_dy, s_down, preferred_element_type=BF),
            jnp.zeros((every, width - 3 * cols), BF),
        ],
        axis=1,
    )
    row_weight_wide = jnp.broadcast_to(flat(row_weight[:, :, None]), (rows, 128))
    chunk, s_chunk = rows // n_tp, every // n_tp
    hidden, grad_gate, grad_up, s_all, dots = call(
        functools.partial(hidden_kernel, n_tp, cols),
        1,
        [
            ((rows, ff), BF),
            ((rows, ff), BF),
            ((rows, ff), BF),
            ((every, width), BF),
            ((n_tp, 8, chunk), F32),
        ],
        [pltpu.VMEM((rows // 2, ff), BF)] * 3
        + [pltpu.VMEM((every // 2, width), BF)]
        + [pltpu.VMEM((rows // 2, ff), BF)] * 3
        + [pltpu.VMEM((every // 2, width), BF)]
        + [pltpu.VMEM((half - 1, chunk, ff), BF)] * 3
        + [pltpu.VMEM((half - 1, s_chunk, width), BF)]
        + [
            dma((4,)), dma((4,)), dma((half - 1, 4)), dma((half - 1, 4)),
            dma((half - 1, 5)), dma((half - 1, 5)), dma((half, 5)), dma((half, 5)),
        ],
        gate_part, up_part, back_part, s_part, row_weight_wide,
    )
    hidden = hidden[:used].reshape(experts, per_expert, ff)
    grad_gate = grad_gate[:used].reshape(experts, per_expert, ff)
    grad_up = grad_up[:used].reshape(experts, per_expert, ff)
    dots = dots[:, 0, :].reshape(rows)[:used].reshape(experts, per_expert)

    weighted = (row_weight[:, :, None] * recv_dy.astype(F32)).astype(BF)
    down_grad = jnp.einsum("erf,erl->efl", hidden, weighted, preferred_element_type=F32)
    gate_wgrad = jnp.einsum("erl,erf->elf", recv_x, grad_gate, preferred_element_type=F32)
    up_wgrad = jnp.einsum("erl,erf->elf", recv_x, grad_up, preferred_element_type=F32)
    row_grad = (
        jnp.einsum("erf,elf->erl", grad_gate, expert_gate, preferred_element_type=F32)
        + jnp.einsum("erf,elf->erl", grad_up, expert_up, preferred_element_type=F32)
    ).astype(BF)
    s_hidden = s_all[:, :cols]
    s_grads = s_all[:, cols : 3 * cols]
    shared_pair = jnp.einsum("tl,ts->ls", all_x, s_grads, preferred_element_type=F32)
    shared_gate_grad, shared_up_grad = shared_pair[:, :cols], shared_pair[:, cols:]
    shared_down_grad = jnp.einsum("ts,tl->sl", s_hidden, all_dy, preferred_element_type=F32)
    token_part = (
        jnp.einsum("ert,erl->tl", onehot, row_grad, preferred_element_type=F32)
        + jnp.einsum("ts,ls->tl", s_grads, s_pair, preferred_element_type=F32)
    ).astype(BF)
    dot_of = jnp.sum(jnp.where(hot, dots[:, :, None], 0.0), axis=1)
    dot_of = dot_of.reshape(experts, n_ep, tok_rows).transpose(1, 0, 2)
    weight_part = jnp.sum(jnp.where(match, dot_of[:, None], 0.0), axis=2)
    weight_part = jnp.pad(weight_part, ((0, 0), (0, up_to(picks, 8) - picks), (0, 0)))
    gate_rows_sq = jnp.sum(gate_wgrad * gate_wgrad, axis=2)
    up_rows_sq = jnp.sum(up_wgrad * up_wgrad, axis=2)
    down_sq = jnp.sum(down_grad * down_grad, axis=2)
    shared_down_sq = jnp.sum(shared_down_grad * shared_down_grad, axis=1)
    over_tp = jnp.concatenate(
        [down_sq, jnp.pad(shared_down_sq, (0, ff - cols))[None]], axis=0
    )
    over_tp = jnp.pad(over_tp, ((0, up_to(experts + 1, 8) - experts - 1), (0, 0)))
    over_ep = jnp.stack(
        [
            jnp.sum(shared_gate_grad * shared_gate_grad, axis=1),
            jnp.sum(shared_up_grad * shared_up_grad, axis=1),
        ]
    )
    over_ep = jnp.pad(over_ep, ((0, 6), (0, 0)))
    peers, t_peers = n_ep - 1, n_tp - 1
    token_grad, weight_grad, over_ep, over_tp = call(
        functools.partial(finish_kernel, n_ep, n_tp),
        2,
        [
            ((tok_rows, narrow), BF),
            (weight_part.shape[1:], F32),
            (over_ep.shape, F32),
            (over_tp.shape, F32),
        ],
        [
            pltpu.VMEM((peers, tok_rows, narrow), BF),
            pltpu.VMEM((peers,) + weight_part.shape[1:], F32),
            pltpu.VMEM((peers,) + over_ep.shape, F32),
            pltpu.VMEM((t_peers,) + over_tp.shape, F32),
            dma((peers, 3)), dma((peers, 3)), dma((t_peers,)), dma((t_peers,)),
        ],
        token_part.reshape(n_ep, tok_rows, narrow), weight_part, over_ep, over_tp,
    )
    return (
        token_grad,
        weight_grad[:picks].T,
        gate_wgrad,
        up_wgrad,
        down_grad,
        shared_gate_grad,
        shared_up_grad,
        shared_down_grad,
        gate_rows_sq,
        up_rows_sq,
        over_tp[:experts],
        over_ep[0],
        over_ep[1],
        over_tp[experts, :cols],
    )


def solution(mesh):
    n_ep, n_tp = mesh.shape["ep"], mesh.shape["tp"]
    return jax.shard_map(
        functools.partial(per_device, n_ep, n_tp),
        mesh=mesh,
        in_specs=(
            P("ep", "tp"),
            P("ep", "tp"),
            P("ep", None),
            P("ep", None),
            P("ep", "tp", None),
            P("ep", "tp", None),
            P("ep", None, "tp"),
            P("tp", None),
            P("tp", None),
            P(None, "tp"),
        ),
        out_specs=(
            P("ep", "tp"),
            P("ep", None),
            P("ep", "tp", None),
            P("ep", "tp", None),
            P("ep", None, "tp"),
            P("tp", "ep"),
            P("tp", "ep"),
            P("ep", "tp"),
            P("ep", "tp"),
            P("ep", "tp"),
            P("ep", None),
            P("tp"),
            P("tp"),
            P("ep"),
        ),
        check_vma=False,
    )
```

```python
import functools

import jax
import jax.numpy as jnp
from jax import lax
from jax.experimental import pallas as pl
from jax.experimental.pallas import tpu as pltpu
from jax.sharding import PartitionSpec as P

BF = jnp.bfloat16
F32 = jnp.float32
MESH = pl.DeviceIdType.MESH
VMEM = pl.BlockSpec(memory_space=pltpu.VMEM)


def up_to(value, unit):
    return (value + unit - 1) // unit * unit


def silu_parts(pre):
    logistic = jax.nn.sigmoid(pre)
    return (pre * logistic, logistic * (1.0 + pre * (1.0 - logistic)))


def remote(src, dst, send, recv, where):
    return pltpu.make_async_remote_copy(
        src_ref=src,
        dst_ref=dst,
        send_sem=send,
        recv_sem=recv,
        device_id=where,
        device_id_type=MESH,
    )


def greet(places):
    barrier = pltpu.get_barrier_semaphore()
    for place in places:
        pl.semaphore_signal(barrier, inc=1, device_id=place, device_id_type=MESH)
    pl.semaphore_wait(barrier, len(places))


def dot(left, right, left_dim, right_dim, precision=None):
    return lax.dot_general(
        left,
        right,
        (((left_dim,), (right_dim,)), ((), ())),
        precision=precision,
        preferred_element_type=F32,
    )


def front_kernel(
    n_ep, n_tp, experts, per_expert, capacity, picks, cols,
    x, dy, meta, w_gate, w_up, w_down, s_in, s_in_back, s_out_w,
    all_x, all_dy, all_meta, oh, recv_x, weighted, hid, gg, gu, so, dots, token_part,
    wg, wu, wd, rw, g, u, b, s, pg, pu, pb, ps, hg, hu, hb, hs, cg, cu, cb, cs,
    w_sem, z_send, z_recv, a_send, a_recv, b_send, b_recv, c_send, c_recv, d_send, d_recv,
):
    ep, me = lax.axis_index("ep"), lax.axis_index("tp")
    half = n_tp // 2
    parity = lax.rem(me, 2)
    mine = me // 2
    partner = {"tp": me + 1 - 2 * parity}
    others = [lax.rem(mine + d, half) for d in range(1, half)]
    places = [{"tp": 2 * j + parity} for j in others]
    eps = [lax.rem(ep + d, n_ep) for d in range(1, n_ep)]
    tok = x.shape[0]
    rows = g.shape[0] // n_tp
    s_rows = s.shape[0] // n_tp
    used = experts * per_expert
    loads = []
    for k, (src, dst) in enumerate(((w_gate, wg), (w_up, wu), (w_down, wd))):
        loads.append(pltpu.make_async_copy(src, dst, w_sem.at[k]))
        loads[-1].start()
    greet([{"ep": p} for p in eps] + [partner] + places)

    blocks = ((meta, all_meta), (x, all_x), (dy, all_dy))
    gathered = [[], [], []]
    for k, (src, dst) in enumerate(blocks):
        for d, p in enumerate(eps):
            c = remote(src, dst.at[ep], z_send.at[d, k], z_recv.at[d, k], {"ep": p})
            c.start()
            gathered[k].append(c)
    for src, dst in blocks:
        dst[ep] = src[...]
    if used < g.shape[0]:
        oh[...] = jnp.zeros_like(oh)
        rw[...] = jnp.zeros_like(rw)
        for ref in (g, u, b):
            ref[pl.ds(used, g.shape[0] - used), :] = jnp.zeros(
                (g.shape[0] - used, g.shape[1]), F32
            )
    for c in gathered[0]:
        c.wait_recv()
    e_rows = up_to(experts, 8)
    ids = (ep * experts + lax.broadcasted_iota(jnp.int32, (e_rows, tok), 0)).astype(F32)
    before = jnp.where(
        lax.broadcasted_iota(jnp.int32, (tok, tok), 0)
        < lax.broadcasted_iota(jnp.int32, (tok, tok), 1),
        1.0,
        0.0,
    ).astype(BF)
    place_in = lax.broadcasted_iota(jnp.int32, (per_expert, tok), 0).astype(F32)
    sums = [jnp.zeros((per_expert, 1), F32) for _ in range(experts)]
    for blk in range(n_ep):
        info = all_meta[blk]
        chosen = jnp.zeros((e_rows, tok), F32)
        weight_of = jnp.zeros((e_rows, tok), F32)
        for k in range(picks):
            same = info[k : k + 1, :] == ids
            chosen = jnp.where(same, 1.0, chosen)
            weight_of = jnp.where(same, info[picks + k : picks + k + 1, :], weight_of)
        rank = dot(chosen.astype(BF), before, 1, 0)
        slot = jnp.where(chosen > 0.0, rank + float(capacity * blk), -1.0)
        for e in range(experts):
            hot = place_in == slot[e : e + 1, :]
            oh[blk, pl.ds(e * per_expert, per_expert), :] = jnp.where(hot, 1.0, 0.0).astype(BF)
            sums[e] = sums[e] + jnp.sum(
                jnp.where(hot, weight_of[e : e + 1, :], 0.0), axis=1, keepdims=True
            )
    for e in range(experts):
        rw[pl.ds(e * per_expert, per_expert), :] = jnp.broadcast_to(sums[e], (per_expert, 128))

    full = (g, u, b, s)
    got = (pg, pu, pb, ps)
    held = (hg, hu, hb, hs)
    landed = (cg, cu, cb, cs)
    sizes = (rows, rows, rows, s_rows)

    def span(start, size):
        return pl.ds(pl.multiple_of(start * size, size), size)

    first = [None] * 4
    second = [[], [], [], []]

    def swap(k):
        first[k] = remote(
            full[k].at[span(1 - parity, half * sizes[k])],
            got[k],
            a_send.at[k],
            a_recv.at[k],
            partner,
        )
        first[k].start()

    def spread(k):
        first[k].wait()
        held[k][...] = (full[k][span(parity, half * sizes[k]), :] + got[k][...]).astype(BF)
        for d, j in enumerate(others):
            c = remote(
                held[k].at[span(j, sizes[k])],
                landed[k].at[d],
                b_send.at[d, k],
                b_recv.at[d, k],
                places[d],
            )
            c.start()
            second[k].append(c)

    def pick(source):
        total = dot(oh[0], source[0], 1, 0)
        for blk in range(1, n_ep):
            total = total + dot(oh[blk], source[blk], 1, 0)
        return total

    for c in gathered[1]:
        c.wait_recv()
    recv_x[...] = pick(all_x).astype(BF)
    for k, weight in ((0, wg), (1, wu)):
        loads[k].wait()
        for e in range(experts):
            at = pl.ds(e * per_expert, per_expert)
            full[k][at, :] = dot(recv_x[at, :], weight[e], 1, 0)
        swap(k)
    for blk in range(n_ep):
        s[pl.ds(blk * tok, tok), :] = dot(all_x[blk], s_in[...], 1, 1)
    spread(0)
    spread(1)
    for c in gathered[2]:
        c.wait_recv()
    recv_dy = pick(all_dy)
    weighted[...] = (rw[...][:, :1] * recv_dy).astype(BF)
    hid_dy = recv_dy.astype(BF)
    loads[2].wait()
    for e in range(experts):
        b[pl.ds(e * per_expert, per_expert), :] = dot(
            hid_dy[e * per_expert : (e + 1) * per_expert, :], wd[e], 1, 1
        )
    swap(2)
    for blk in range(n_ep):
        s[pl.ds(blk * tok, tok), :] += dot(all_dy[blk], s_in_back[...], 1, 1)
    swap(3)
    spread(2)
    spread(3)

    place = parity * half + mine

    def total(k):
        for c in second[k]:
            c.wait_recv()
        out = full[k][span(place, sizes[k]), :] + got[k][span(mine, sizes[k]), :]
        for d in range(half - 1):
            out = out + landed[k][d].astype(F32)
        return out

    last = []

    def share(k, ref, where):
        block = ref.at[where]
        for d in range(half - 1):
            c = remote(block, block, c_send.at[d, k], c_recv.at[d, k], places[d])
            c.start()
            last.append(c)
        c = remote(block, block, d_send.at[0, k], d_recv.at[0, k], partner)
        c.start()
        last.append(c)

    outs = ((hid, rows), (gg, rows), (gu, rows), (dots, 1), (so, s_rows))

    def part(k, index):
        return pl.ds(index, 1) if k == 3 else span(index, outs[k][1])

    gate, up, back = total(0), total(1), total(2)
    silu_out, silu_slope = silu_parts(gate)
    hidden = (silu_out * up).astype(BF)
    mine_rows = span(place, rows)
    dhidden = rw[mine_rows, :][:, :1] * back
    hid[mine_rows, :] = hidden
    gg[mine_rows, :] = (dhidden * up * silu_slope).astype(BF)
    gu[mine_rows, :] = (dhidden * silu_out).astype(BF)
    dots[place] = dot(
        jnp.ones((8, gate.shape[1]), F32),
        hidden.astype(F32) * back,
        1,
        1,
        lax.Precision.HIGHEST,
    )
    for k in range(4):
        share(k, outs[k][0], part(k, place))

    both = total(3)
    width = both.shape[1]
    lane = lax.broadcasted_iota(jnp.int32, both.shape, 1)
    s_up = pltpu.roll(both, width - cols, 1)
    s_back = pltpu.roll(both, width - 2 * cols, 1)
    s_out, s_slope = silu_parts(both)
    s_dgate = pltpu.roll(s_back * s_up * s_slope, cols, 1)
    s_dup = pltpu.roll(s_back * s_out, 2 * cols, 1)
    so[span(place, s_rows), :] = jnp.where(
        lane < cols, s_out * s_up, jnp.where(lane < 2 * cols, s_dgate, s_dup)
    ).astype(BF)
    share(4, so, part(4, place))

    def forward(k):
        ref = outs[k][0]
        for d in range(half - 1):
            source = lax.rem(mine + half - 1 - d, half)
            block = ref.at[part(k, parity * half + source)]
            remote(
                block, block, c_send.at[d, k], c_recv.at[d, k], places[d]
            ).wait_recv()
            c = remote(block, block, d_send.at[1 + d, k], d_recv.at[1 + d, k], partner)
            c.start()
            last.append(c)

    def settle(k):
        ref = outs[k][0]
        for d in range(half):
            source = mine if d == 0 else lax.rem(mine + half - d, half)
            block = ref.at[part(k, (1 - parity) * half + source)]
            remote(block, block, d_send.at[d, k], d_recv.at[d, k], partner).wait_recv()

    for k in range(4):
        forward(k)
    for k in range(4):
        settle(k)
    row_grad = []
    for e in range(experts):
        at = pl.ds(e * per_expert, per_expert)
        row_grad.append(
            (dot(gg[at, :], wg[e], 1, 1) + dot(gu[at, :], wu[e], 1, 1)).astype(BF)
        )
    if used < g.shape[0]:
        row_grad.append(jnp.zeros((g.shape[0] - used, x.shape[1]), BF))
    row_grad = jnp.concatenate(row_grad, axis=0)
    forward(4)
    settle(4)
    for blk in range(n_ep):
        token_part[blk] = (
            dot(oh[blk], row_grad, 0, 0)
            + dot(so[pl.ds(blk * tok, tok), :], s_out_w[...], 1, 0)
        ).astype(BF)
    for group in second:
        for c in group:
            c.wait_send()
    for group in gathered:
        for c in group:
            c.wait_send()
    for c in last:
        c.wait_send()


def row_squares(square):
    ones = jnp.ones((8, square.shape[1]), BF)
    high = square.astype(BF)
    low = (square - high.astype(F32)).astype(BF)
    return (dot(ones, high, 1, 1) + dot(ones, low, 1, 1))[:1, :]


def weights_kernel(
    experts, cols,
    recv_x, weighted, hid, gg, gu, all_x, all_dy, so,
    gate_out, up_out, down_out, sg_out, su_out, sd_out, gate_sq, up_sq, over_tp, over_ep,
):
    e = pl.program_id(0)
    gate = dot(recv_x[...], gg[...], 0, 0)
    gate_out[0] = gate
    gate_sq[pl.ds(e, 1), :] = row_squares(gate * gate)
    up = dot(recv_x[...], gu[...], 0, 0)
    up_out[0] = up
    up_sq[pl.ds(e, 1), :] = row_squares(up * up)
    down = dot(hid[...], weighted[...], 0, 0)
    down_out[0] = down

    @pl.when(e == 0)
    def _():
        over_tp[...] = jnp.zeros_like(over_tp)
        over_ep[...] = jnp.zeros_like(over_ep)
        pair = dot(so[...], all_x[...], 0, 0)
        sg, su = pair[cols : 2 * cols, :], pair[2 * cols : 3 * cols, :]
        sg_out[...] = sg
        su_out[...] = su
        over_ep[0:1, :] = jnp.sum(sg * sg, axis=0, keepdims=True)
        over_ep[1:2, :] = jnp.sum(su * su, axis=0, keepdims=True)
        sd_full = dot(so[...], all_dy[...], 0, 0)
        sd_out[...] = sd_full[:cols, :]
        sq = row_squares(sd_full * sd_full)
        kept = lax.broadcasted_iota(jnp.int32, sq.shape, 1) < cols
        sq = jnp.where(kept, sq, 0.0)
        span = min(over_tp.shape[1], sq.shape[1])
        over_tp[experts : experts + 1, :span] = sq[:, :span]

    over_tp[pl.ds(e, 1), :] = row_squares(down * down)


def finish_kernel(
    n_ep, n_tp, wg, es, ts, wg_out, es_out, ts_out,
    wg_in, es_in, ts_in, e_send, e_recv, t_send, t_recv,
):
    ep, tp = lax.axis_index("ep"), lax.axis_index("tp")
    eps = [lax.rem(ep + d, n_ep) for d in range(1, n_ep)]
    tps = [lax.rem(tp + d, n_tp) for d in range(1, n_tp)]
    greet([{"ep": p} for p in eps] + [{"tp": p} for p in tps])
    copies = []
    for d, p in enumerate(eps):
        for k, (src, dst) in enumerate(((wg.at[p], wg_in.at[d]), (es, es_in.at[d]))):
            copies.append(remote(src, dst, e_send.at[d, k], e_recv.at[d, k], {"ep": p}))
            copies[-1].start()
    for d, p in enumerate(tps):
        copies.append(remote(ts, ts_in.at[d], t_send.at[d], t_recv.at[d], {"tp": p}))
        copies[-1].start()
    for c in copies:
        c.wait()
    weights = wg[ep]
    norms = es[...]
    for d in range(n_ep - 1):
        weights = weights + wg_in[d]
        norms = norms + es_in[d]
    wg_out[...] = weights
    es_out[...] = norms
    down = ts[...]
    for d in range(n_tp - 1):
        down = down + ts_in[d]
    ts_out[...] = down


def call(kernel, collective, outs, scratch, *args, specs=None):
    return pl.pallas_call(
        kernel,
        out_shape=[jax.ShapeDtypeStruct(s, t) for s, t in outs],
        in_specs=specs or [VMEM] * len(args),
        out_specs=[VMEM] * len(outs),
        scratch_shapes=scratch,
        compiler_params=pltpu.CompilerParams(
            collective_id=collective,
            has_side_effects=True,
            vmem_limit_bytes=48 * 1024 * 1024,
        ),
    )(*args)


def per_device(
    n_ep, n_tp,
    tokens, cotangent, routes, gate_weights,
    expert_gate, expert_up, expert_down,
    shared_gate, shared_up, shared_down,
):
    dma = pltpu.SemaphoreType.DMA
    half = n_tp // 2
    tok_rows, narrow = tokens.shape
    picks = routes.shape[1]
    experts, _, ff = expert_gate.shape
    experts_all = experts * n_ep
    capacity = max(2, (tok_rows * picks + experts_all - 1) // experts_all)
    every = tok_rows * n_ep
    cols = shared_gate.shape[1] // n_ep
    ep = lax.axis_index("ep")
    per_expert = up_to(capacity * n_ep, 16)
    used = experts * per_expert
    rows = up_to(used, 16 * n_tp)
    width = up_to(3 * cols, 128)
    chunk, s_chunk = rows // n_tp, every // n_tp

    meta = jnp.concatenate([routes.astype(F32).T, gate_weights.T], axis=0)
    meta = jnp.pad(meta, ((0, up_to(2 * picks, 8) - 2 * picks), (0, 0)))
    sg = lax.dynamic_slice_in_dim(shared_gate.T, ep * cols, cols, 0)
    su = lax.dynamic_slice_in_dim(shared_up.T, ep * cols, cols, 0)
    sd = lax.dynamic_slice_in_dim(shared_down, ep * cols, cols, 0)
    s_in = jnp.pad(jnp.concatenate([sg, su], axis=0), ((0, width - 2 * cols), (0, 0)))
    s_in_back = jnp.pad(sd, ((2 * cols, width - 3 * cols), (0, 0)))
    s_out_w = jnp.pad(jnp.concatenate([sg, su], axis=0), ((cols, width - 3 * cols), (0, 0)))
    anywhere = pl.BlockSpec(memory_space=pl.ANY)
    vm = pltpu.VMEM
    (
        all_x, all_dy, all_meta, onehot, recv_x, weighted,
        hidden, grad_gate, grad_up, s_all, dots, token_part,
    ) = call(
        functools.partial(
            front_kernel, n_ep, n_tp, experts, per_expert, capacity, picks, cols
        ),
        0,
        [
            ((n_ep, tok_rows, narrow), BF),
            ((n_ep, tok_rows, narrow), BF),
            ((n_ep,) + meta.shape, F32),
            ((n_ep, rows, tok_rows), BF),
            ((rows, narrow), BF),
            ((rows, narrow), BF),
            ((rows, ff), BF),
            ((rows, ff), BF),
            ((rows, ff), BF),
            ((every, width), BF),
            ((n_tp, 8, chunk), F32),
            ((n_ep, tok_rows, narrow), BF),
        ],
        [
            vm(expert_gate.shape, BF), vm(expert_up.shape, BF), vm(expert_down.shape, BF),
            vm((rows, 128), F32),
        ]
        + [vm((rows, ff), F32)] * 3 + [vm((every, width), F32)]
        + [vm((rows // 2, ff), F32)] * 3 + [vm((every // 2, width), F32)]
        + [vm((rows // 2, ff), BF)] * 3 + [vm((every // 2, width), BF)]
        + [vm((half - 1, chunk, ff), BF)] * 3 + [vm((half - 1, s_chunk, width), BF)]
        + [
            dma((3,)), dma((n_ep - 1, 3)), dma((n_ep - 1, 3)),
            dma((4,)), dma((4,)), dma((half - 1, 4)), dma((half - 1, 4)),
            dma((half - 1, 5)), dma((half - 1, 5)), dma((half, 5)), dma((half, 5)),
        ],
        tokens, cotangent, meta, expert_gate, expert_up, expert_down,
        s_in, s_in_back, s_out_w,
        specs=[VMEM] * 3 + [anywhere] * 3 + [VMEM] * 3,
    )
    token_grad = token_part[ep].astype(F32)
    for d in range(1, n_ep):
        moved = lax.ppermute(
            lax.dynamic_index_in_dim(token_part, lax.rem(ep + d, n_ep), 0, False),
            "ep",
            [(i, (i + d) % n_ep) for i in range(n_ep)],
        )
        token_grad = token_grad + moved.astype(F32)
    token_grad = token_grad.astype(BF)

    whole_x = all_x.reshape(every, narrow)
    whole_dy = all_dy.reshape(every, narrow)
    norm_rows = up_to(experts + 1, 8)

    def fixed(shape):
        return pl.BlockSpec(shape, lambda e: (0,) * len(shape))

    def rowed(columns):
        return pl.BlockSpec((per_expert, columns), lambda e: (e, 0))

    def stacked(a, c):
        return pl.BlockSpec((1, a, c), lambda e: (e, 0, 0))

    flops = 2 * experts * per_expert * narrow * ff * 3 + 4 * every * narrow * width
    (
        gate_wgrad, up_wgrad, down_grad, sg_grad, su_grad, sd_grad,
        gate_rows_sq, up_rows_sq, over_tp, over_ep,
    ) = pl.pallas_call(
        functools.partial(weights_kernel, experts, cols),
        grid=(experts,),
        in_specs=[rowed(narrow), rowed(narrow), rowed(ff), rowed(ff), rowed(ff)]
        + [fixed(whole_x.shape), fixed(whole_dy.shape), fixed(s_all.shape)],
        out_specs=[stacked(narrow, ff), stacked(narrow, ff), stacked(ff, narrow)]
        + [fixed((cols, narrow))] * 3
        + [fixed((experts, narrow))] * 2
        + [fixed((norm_rows, ff)), fixed((8, narrow))],
        out_shape=[
            jax.ShapeDtypeStruct(shape, F32)
            for shape in (
                (experts, narrow, ff), (experts, narrow, ff), (experts, ff, narrow),
                (cols, narrow), (cols, narrow), (cols, narrow),
                (experts, narrow), (experts, narrow), (norm_rows, ff), (8, narrow),
            )
        ],
        cost_estimate=pl.CostEstimate(
            flops=flops, bytes_accessed=experts * narrow * ff * 12, transcendentals=0
        ),
        compiler_params=pltpu.CompilerParams(
            dimension_semantics=("arbitrary",), vmem_limit_bytes=48 * 1024 * 1024
        ),
    )(recv_x, weighted, hidden, grad_gate, grad_up, whole_x, whole_dy, s_all)

    ids = (ep * experts + jnp.arange(experts, dtype=jnp.int32)).astype(F32)
    match = all_meta[:, :picks, None, :] == ids[None, None, :, None]
    hot = onehot[:, :used].reshape(n_ep, experts, per_expert, tok_rows)
    row_dots = dots[:, 0, :].reshape(rows)[:used].reshape(1, experts, per_expert, 1)
    dot_of = jnp.sum(hot.astype(F32) * row_dots, axis=2)
    weight_part = jnp.sum(jnp.where(match, dot_of[:, None], 0.0), axis=2)
    weight_part = jnp.pad(weight_part, ((0, 0), (0, up_to(picks, 8) - picks), (0, 0)))
    peers, t_peers = n_ep - 1, n_tp - 1
    weight_grad, over_ep, over_tp = call(
        functools.partial(finish_kernel, n_ep, n_tp),
        1,
        [(weight_part.shape[1:], F32), (over_ep.shape, F32), (over_tp.shape, F32)],
        [
            vm((peers,) + weight_part.shape[1:], F32),
            vm((peers,) + over_ep.shape, F32),
            vm((t_peers,) + over_tp.shape, F32),
            dma((peers, 2)), dma((peers, 2)), dma((t_peers,)), dma((t_peers,)),
        ],
        weight_part, over_ep, over_tp,
    )
    return (
        token_grad,
        weight_grad[:picks].T,
        gate_wgrad,
        up_wgrad,
        down_grad,
        sg_grad.T,
        su_grad.T,
        sd_grad,
        gate_rows_sq,
        up_rows_sq,
        over_tp[:experts],
        over_ep[0],
        over_ep[1],
        over_tp[experts, :cols],
    )


def solution(mesh):
    n_ep, n_tp = mesh.shape["ep"], mesh.shape["tp"]
    return jax.shard_map(
        functools.partial(per_device, n_ep, n_tp),
        mesh=mesh,
        in_specs=(
            P("ep", "tp"),
            P("ep", "tp"),
            P("ep", None),
            P("ep", None),
            P("ep", "tp", None),
            P("ep", "tp", None),
            P("ep", None, "tp"),
            P("tp", None),
            P("tp", None),
            P(None, "tp"),
        ),
        out_specs=(
            P("ep", "tp"),
            P("ep", None),
            P("ep", "tp", None),
            P("ep", "tp", None),
            P("ep", None, "tp"),
            P("tp", "ep"),
            P("tp", "ep"),
            P("ep", "tp"),
            P("ep", "tp"),
            P("ep", "tp"),
            P("ep", None),
            P("tp"),
            P("tp"),
            P("ep"),
        ),
        check_vma=False,
    )
```
